32 devices in a mesh: fs: 8 (over z, y), tp: 4 (over x, core).
Axes of the slice: x: 2, y: 2, z: 4, core: 2. Of those that a mesh axis runs over, the one named last changes fastest.
Arguments:
- tokens: bfloat16 [4096, 2048], P(('fs', 'tp')), may hold values from -6 to 6
- norm_one: float32 [2048], replicated, may hold values from 0.1 to 1.9
- gate_one: bfloat16 [2048, 4608], P('fs', 'tp'), may hold values from -0.125 to 0.125
- up_one: bfloat16 [2048, 4608], P('fs', 'tp'), may hold values from -0.125 to 0.125
- down_one: bfloat16 [4608, 2048], P('tp', 'fs'), may hold values from -0.1875 to 0.1875
- norm_two: float32 [2048], replicated, may hold values from 0.1 to 1.9
- gate_two: bfloat16 [2048, 4608], P('fs', 'tp'), may hold values from -0.125 to 0.125
- up_two: bfloat16 [2048, 4608], P('fs', 'tp'), may hold values from -0.125 to 0.125
- down_two: bfloat16 [4608, 2048], P('tp', 'fs'), may hold values from -0.1875 to 0.1875
Outputs:
- result: bfloat16 [4096, 2048], P(('fs', 'tp'))
The draws below stay inside these ranges and needn't reach their ends.
All inputs are finite; a program needn't handle non-finite values.
Results may differ from the reference program's by a relative error of at most 0.015.
Values may be sent and summed in bfloat16 or wider, within the bound.
No kernel may reach another device: no remote copies, remote signals or barrier semaphores. Data moves between devices by JAX's collectives and lax.ppermute only.
A program may use at most 64 MiB of HBM per device.

```python
import jax
import jax.numpy as jnp
from jax import lax

D = 2048
FF = 4608
TOKENS = 4096
N_FS = 8
N_TP = 4


def block_scale(stream_key, dims, pieces, least, largest):
    factor_of = 1.0
    for axis_at, parts in pieces:
        steps = jax.random.uniform(jax.random.fold_in(jax.random.fold_in(stream_key, 6), axis_at), (parts,), jnp.float32, least / len(pieces), largest / len(pieces))
        factor_of = factor_of * jnp.repeat(jnp.exp(steps), dims[axis_at] // parts).reshape((-1,) + (1,) * (len(dims) - 1 - axis_at))
    return factor_of


def bell_draw(own_key, dims, scale, bound, split=(), dtype=jnp.bfloat16):
    level = block_scale(own_key, dims, split, -0.22, 0.18) if split else 1.0
    drawn = jax.random.normal(own_key, dims, jnp.float32) * scale * level
    return jnp.minimum(jnp.maximum(drawn, -bound), bound).astype(dtype)


def setup_inputs(seed: int = 0) -> dict:
    key_list = jax.random.split(jax.random.key(seed), 10)
    return {
        "tokens": bell_draw(key_list[0], (TOKENS, D), 1.0, 6.0, ((0, 32),)),
        "norm_one": jnp.clip(1.0 + 0.18 * jax.random.normal(key_list[1], (D,), jnp.float32), 0.1, 1.9),
        "gate_one": bell_draw(key_list[2], (D, FF), D ** -0.5, 0.125, ((0, 8), (1, 4))),
        "up_one": bell_draw(key_list[3], (D, FF), D ** -0.5, 0.125, ((0, 8), (1, 4))),
        "down_one": bell_draw(key_list[4], (FF, D), (FF // 4) ** -0.5, 0.1875, ((0, 4), (1, 8))),
        "norm_two": jnp.clip(1.0 + 0.18 * jax.random.normal(key_list[5], (D,), jnp.float32), 0.1, 1.9),
        "gate_two": bell_draw(key_list[6], (D, FF), D ** -0.5, 0.125, ((0, 8), (1, 4))),
        "up_two": bell_draw(key_list[7], (D, FF), D ** -0.5, 0.125, ((0, 8), (1, 4))),
        "down_two": bell_draw(key_list[8], (FF, D), (FF // 4) ** -0.5, 0.1875, ((0, 4), (1, 8))),
    }


eps = 1e-06

def normalize(rows, gain):
    values = rows.astype(jnp.float32)
    scaled = values * lax.rsqrt(lax.optimization_barrier(jnp.mean(values * values, axis=-1, keepdims=True)) + eps)
    return (scaled * gain.astype(jnp.float32)).astype(jnp.bfloat16)

def product(left, right):
    return jnp.dot(left.astype(jnp.float32), right.astype(jnp.float32), preferred_element_type=jnp.float32)

def half_step(rows, gain, gate_w, up_w, down_w):
    normed = normalize(rows, gain)
    hidden = (jax.nn.silu(product(normed, gate_w)) * product(normed, up_w)).astype(jnp.bfloat16)
    width = down_w.shape[0] // N_TP
    total = jnp.zeros((rows.shape[0], down_w.shape[1]), jnp.float32)
    for block in range(N_TP):
        partial_value = product(hidden[:, block * width:(block + 1) * width], down_w[block * width:(block + 1) * width])
        rounded = lax.optimization_barrier(partial_value.astype(jnp.bfloat16))
        total = total + rounded.astype(jnp.float32)
    return (rows.astype(jnp.float32) + 0.5 * total).astype(jnp.bfloat16)

def reference(tokens, norm_one, gate_one, up_one, down_one, norm_two, gate_two, up_two, down_two):

    def group_step(rows):
        middle = half_step(rows, norm_one, gate_one, up_one, down_one)
        return half_step(middle, norm_two, gate_two, up_two, down_two)
    grouped = tokens.reshape(N_FS, tokens.shape[0] // N_FS, tokens.shape[1])
    return lax.map(group_step, grouped).reshape(tokens.shape)
```

```python
import jax
import jax.numpy as jnp
from jax import lax
from jax.sharding import PartitionSpec as P

eps = 1e-06
AXES = ("fs", "tp")


class Layout:
    def __init__(self, n_fs, n_tp):
        self.c = 2 if n_fs % 2 == 0 and n_tp % 2 == 0 else 1
        self.x = n_tp // self.c
        rest = n_fs // self.c
        self.b = self.x if rest % self.x == 0 else 1
        self.a = rest // self.b
        self.n_tp = n_tp

    def pairs(self, move):
        out = []
        for a in range(self.a):
            for q in range(self.c):
                for b in range(self.b):
                    for x in range(self.x):
                        for c in range(self.c):
                            out.append((self.index(a, q, b, x, c), self.index(*move(a, q, b, x, c))))
        return out

    def index(self, a, q, b, x, c):
        a, q, b, x, c = a % self.a, q % self.c, b % self.b, x % self.x, c % self.c
        return ((a * self.c + q) * self.b + b) * self.n_tp + x * self.c + c

    def send(self, value, move):
        return lax.ppermute(value, AXES, self.pairs(move))


def normalize(rows, gain):
    values = rows.astype(jnp.float32)
    scaled = values * lax.rsqrt(jnp.mean(values * values, axis=-1, keepdims=True) + eps)
    return (scaled * gain).astype(jnp.bfloat16)


def gather_weight(lay, shard):
    lines = [lay.send(shard, lambda a, q, b, x, c, i=i: (a + i, c, b, x, q)) for i in range(lay.a)]
    pieces = []
    for line in lines:
        for j in range(lay.b):
            own = lay.send(line, lambda a, q, b, x, c, j=j: (a, q, b + j, x, c)) if j else line
            pieces.append(own)
            for k in range(1, lay.c):
                pieces.append(lay.send(own, lambda a, q, b, x, c, k=k: (a, q, b, x, c + k)))
    return pieces


def piece_starts(lay):
    f, t = lax.axis_index("fs"), lax.axis_index("tp")
    a, b, c = f // (lay.c * lay.b), f % lay.b, t % lay.c
    return [
        (((a - i) % lay.a) * lay.c + (c - k) % lay.c) * lay.b + (b - j) % lay.b
        for i in range(lay.a)
        for j in range(lay.b)
        for k in range(lay.c)
    ]


def piece_places(lay):
    f, t = lax.axis_index("fs"), lax.axis_index("tp")
    a, b, c = f // (lay.c * lay.b), f % lay.b, t % lay.c
    return [
        (((a - i) % lay.a) * lay.b + (b - j) % lay.b) * lay.c + (c - k) % lay.c
        for i in range(lay.a)
        for k in range(lay.c)
        for j in range(lay.b)
    ]


def columns_at(values, places, width):
    return jnp.concatenate(
        [lax.dynamic_slice_in_dim(values, place * width, width, values.ndim - 1) for place in places], -1
    )


def gather_tokens(lay, rows):
    out = []
    for dq in range(lay.c):
        line = lay.send(rows, lambda a, q, b, x, c: (a, q + dq, b, x, c)) if dq else rows
        for dx in range(lay.x):
            out.append(lay.send(line, lambda a, q, b, x, c: (a, q, b, x + dx, c)) if dx else line)
    return out


def half_step(lay, rows, gain, gate, up, down):
    blocks = gather_tokens(lay, normalize(rows, gain))
    normed = jnp.concatenate(blocks, 0)
    gate_sum = jnp.dot(normed, jnp.concatenate(gate, 0), preferred_element_type=jnp.float32)
    up_sum = jnp.dot(normed, jnp.concatenate(up, 0), preferred_element_type=jnp.float32)
    hidden = (jax.nn.silu(gate_sum) * up_sum).astype(jnp.bfloat16)
    terms = jnp.dot(hidden, jnp.concatenate(down, 1), preferred_element_type=jnp.float32).astype(jnp.bfloat16)
    n = rows.shape[0]
    total = terms[:n].astype(jnp.float32)
    at = 0
    for dq in range(lay.c):
        for dx in range(lay.x):
            if dq or dx:
                got = lay.send(terms[at : at + n], lambda a, q, b, x, c: (a, q - dq, b, x - dx, c))
                total = total + got.astype(jnp.float32)
            at += n
    return (rows.astype(jnp.float32) + 0.5 * total).astype(jnp.bfloat16)


def solution(mesh):
    lay = Layout(mesh.shape["fs"], mesh.shape["tp"])

    def on_device(tokens, norm_one, gate_one, up_one, down_one, norm_two, gate_two, up_two, down_two):
        width = tokens.shape[1] // mesh.shape["fs"]
        starts, places = piece_starts(lay), piece_places(lay)
        rows = columns_at(tokens, starts, width)
        first = [gather_weight(lay, w) for w in (gate_one, up_one, down_one)]
        second = [gather_weight(lay, w) for w in (gate_two, up_two, down_two)]
        middle = half_step(lay, rows, columns_at(norm_one, starts, width), *first)
        result = half_step(lay, middle, columns_at(norm_two, starts, width), *second)
        return columns_at(result, places, width)

    return jax.shard_map(
        on_device,
        mesh=mesh,
        in_specs=(
            P(("fs", "tp"), None),
            P(),
            P("fs", "tp"),
            P("fs", "tp"),
            P("tp", "fs"),
            P(),
            P("fs", "tp"),
            P("fs", "tp"),
            P("tp", "fs"),
        ),
        out_specs=P(("fs", "tp"), None),
        check_vma=False,
    )
```
